128 devices in a mesh: dp: 4 (over x), kv: 16 (over z, y), tp: 2 (over core).
Axes of the slice: x: 4, y: 4, z: 4, core: 2. Of those that a mesh axis runs over, the one named last changes fastest.
Arguments:
- layer_input: bfloat16 [512, 4096], P('dp', ('kv', 'tp')), parts along dimension 0, may hold values from -22 to 22
- gate_weight: bfloat16 [4096, 2048], P(('kv', 'tp')), may hold values from -0.09375 to 0.09375
- value_weight: bfloat16 [4096, 2048], P(('kv', 'tp')), may hold values from -0.09375 to 0.09375
- write_weight: bfloat16 [4096, 256], P(('kv', 'tp')), may hold values from -0.09375 to 0.09375
- read_weight: bfloat16 [4096, 256], P(('kv', 'tp')), may hold values from -0.09375 to 0.09375
- step_weight: bfloat16 [4096, 32], P(('kv', 'tp')), may hold values from -0.09375 to 0.09375
- value_taps: bfloat16 [4, 2048], replicated, may hold values from -3 to 3
- write_taps: bfloat16 [4, 256], replicated, may hold values from -3 to 3
- read_taps: bfloat16 [4, 256], replicated, may hold values from -3 to 3
- past_values: bfloat16 [512, 3, 2048], P(('dp', 'kv', 'tp')), parts along dimension 0, may hold values from -6 to 6
- past_writes: bfloat16 [512, 3, 256], P(('dp', 'kv', 'tp')), parts along dimension 0, may hold values from -6 to 6
- past_reads: bfloat16 [512, 3, 256], P(('dp', 'kv', 'tp')), parts along dimension 0, may hold values from -6 to 6
- step_bias: float32 [32], replicated, may hold values from -4 to -1
- decay_log: float32 [32], replicated, may hold values from 0 to 2.77
- skip_scale: float32 [32], replicated, may hold values from 0.5 to 2
- state_past: float32 [512, 32, 64, 128], P(('dp', 'kv', 'tp')), parts along dimension 0, may hold values from -3 to 3
- mixer_gain: float32 [2048], replicated, may hold values from 0.1 to 1.9
- out_weight: bfloat16 [2048, 4096], P(None, ('kv', 'tp')), may hold values from -0.125 to 0.125
- norm1_gain: float32 [4096], replicated, may hold values from 0.24 to 3.7
- up_weight: bfloat16 [4096, 16384], P(None, ('kv', 'tp')), may hold values from -0.09375 to 0.09375
- down_weight: bfloat16 [16384, 4096], P(('kv', 'tp')), may hold values from -0.09375 to 0.09375
- norm2_gain: float32 [4096], replicated, may hold values from 0.1 to 1.9
Outputs:
- layer_output: bfloat16 [512, 4096], P('dp', ('kv', 'tp')), parts along dimension 0
- state_next: float32 [512, 32, 64, 128], P(('dp', 'kv', 'tp')), parts along dimension 0
The draws below stay inside these ranges and needn't reach their ends.
There are 4 independent parts, one for each index of `dp`. The reference program is written for one: setup_inputs(seed, part) draws one part's arguments, and reference() takes and returns one part's arrays. A program takes and returns all parts, laid end to end along the dimension named above; an argument that names none is the same for every part. Nothing has to cross between parts.
All inputs are finite; a program needn't handle non-finite values.
Results may differ from the reference program's by a relative error of at most 0.012.
Values may be sent and summed in bfloat16 or wider, within the bound.
No kernel may reach another device: no remote copies, remote signals or barrier semaphores. Data moves between devices by JAX's collectives and lax.ppermute only.
A program may use at most 64 MiB of HBM per device.

```python
import math
import jax
import jax.numpy as jnp
from jax import lax

D = 4096
HEADS = 32
HEAD_DIM = 64
STATE_DIM = 128
GROUPS = 2
CONV_TAPS = 4
FF = 16384
INNER = 2048
SEQS = 128


def draw_layer_input(key, part):
    first_key, second_key = jax.random.split(jax.random.fold_in(key, 11), 2)
    ramp = jnp.exp(jnp.linspace(math.log(0.4), math.log(2.5), D)).astype(jnp.float32)
    rough = jnp.exp(jax.random.uniform(second_key, (D,), jnp.float32, -0.35, 0.35))
    base = jnp.clip(jax.random.normal(first_key, (SEQS, D), jnp.float32), -6.0, 6.0)
    return (base * ramp[None, :] * rough[None, :]).astype(jnp.bfloat16)


def draw_norm1_gain(key, part):
    first_key = jax.random.fold_in(key, 23)
    ramp = jnp.exp(jnp.linspace(math.log(0.4), math.log(2.5), D)).astype(jnp.float32)
    rough = jnp.exp(jax.random.uniform(first_key, (D,), jnp.float32, -0.2, 0.2))
    return (ramp * rough).astype(jnp.float32)


def with_spikes(entries, own_key, source, target, parts, factor):
    def block_of(dim):
        return (jnp.arange(entries.shape[dim]) // (entries.shape[dim] // parts)).reshape((-1,) + (1,) * (entries.ndim - 1 - dim))

    near = jax.random.permutation(own_key, parts)[block_of(target)]
    other_side = (block_of(target) + parts // 2) % parts
    return jnp.where((block_of(source) == near) | (block_of(source) == other_side), factor * entries, entries)


def steps_of(rng, shape, cuts, smallest, high):
    def one(dim, shards_of):
        steps = jax.random.uniform(jax.random.fold_in(jax.random.fold_in(rng, 6), dim), (shards_of,), jnp.float32, smallest / len(cuts), high / len(cuts))
        return jnp.repeat(jnp.exp(steps), shape[dim] // shards_of).reshape((-1,) + (1,) * (len(shape) - dim - 1))

    level = one(*cuts[0])
    for cut in cuts[1:]:
        level = level * one(*cut)
    return level


def normal_values(rng, extent, spread, most, cuts=(), kind=jnp.bfloat16):
    values = spread * jax.random.normal(rng, extent, jnp.float32)
    if cuts:
        values = values * steps_of(rng, extent, cuts, -0.22, 0.18)
    return jnp.clip(values, -most, most).astype(kind)


def gaussian_with(stream_key, dims, width, bound, shards, heavy, kind=jnp.bfloat16):
    values = width * jax.random.normal(stream_key, dims, jnp.float32)
    if shards:
        values = values * steps_of(stream_key, dims, shards, -0.22, 0.18)
    return jnp.clip(with_spikes(values, jax.random.fold_in(stream_key, 3), *heavy), -bound, bound).astype(kind)


def setup_inputs(seed: int = 0, part: int = 0) -> dict:
    key_of = jax.random.split(jax.random.key(seed), 23)
    own_keys = jax.random.split(jax.random.fold_in(key_of[22], part), 23)
    return {
        "layer_input": draw_layer_input(jax.random.fold_in(jax.random.fold_in(key_of[22], part), 71), part),
        "gate_weight": normal_values(key_of[1], (D, INNER), D ** -0.5, 0.09375, ((0, 32),)),
        "value_weight": normal_values(key_of[2], (D, INNER), D ** -0.5, 0.09375, ((0, 32),)),
        "write_weight": normal_values(key_of[3], (D, GROUPS * STATE_DIM), D ** -0.5, 0.09375, ((0, 32),)),
        "read_weight": normal_values(key_of[4], (D, GROUPS * STATE_DIM), D ** -0.5, 0.09375, ((0, 32),)),
        "step_weight": normal_values(key_of[5], (D, HEADS), D ** -0.5, 0.09375, ((0, 32),)),
        "value_taps": normal_values(key_of[6], (CONV_TAPS, INNER), CONV_TAPS ** -0.5, 3.0),
        "write_taps": normal_values(key_of[7], (CONV_TAPS, GROUPS * STATE_DIM), CONV_TAPS ** -0.5, 3.0),
        "read_taps": normal_values(key_of[8], (CONV_TAPS, GROUPS * STATE_DIM), CONV_TAPS ** -0.5, 3.0),
        "past_values": normal_values(own_keys[9], (SEQS, CONV_TAPS - 1, INNER), 1.0, 6.0, ((0, 32),)),
        "past_writes": normal_values(own_keys[10], (SEQS, CONV_TAPS - 1, GROUPS * STATE_DIM), 1.0, 6.0, ((0, 32),)),
        "past_reads": normal_values(own_keys[11], (SEQS, CONV_TAPS - 1, GROUPS * STATE_DIM), 1.0, 6.0, ((0, 32),)),
        "step_bias": jnp.clip(jax.random.uniform(key_of[12], (HEADS,), jnp.float32, -4.0, -1.0), -4.0, -1.0),
        "decay_log": jnp.clip(jax.random.uniform(key_of[13], (HEADS,), jnp.float32, 0.0, 2.77), 0.0, 2.77),
        "skip_scale": jnp.clip(jnp.exp(jax.random.uniform(key_of[14], (HEADS,), jnp.float32, math.log(0.5), math.log(2.0))), 0.5, 2.0),
        "state_past": normal_values(own_keys[15], (SEQS, HEADS, HEAD_DIM, STATE_DIM), 0.5, 3.0, ((0, 32),), jnp.float32),
        "mixer_gain": jnp.clip(1.0 + 0.18 * jax.random.normal(key_of[16], (INNER,), jnp.float32), 0.1, 1.9),
        "out_weight": normal_values(key_of[17], (INNER, D), INNER ** -0.5, 0.125, ((1, 32),)),
        "norm1_gain": draw_norm1_gain(jax.random.fold_in(key_of[22], 71), part),
        "up_weight": normal_values(key_of[19], (D, FF), D ** -0.5, 0.09375, ((1, 32),)),
        "down_weight": gaussian_with(key_of[20], (FF, D), FF ** -0.5, 0.09375, ((0, 32),), (0, 1, 32, 2.75)),
        "norm2_gain": jnp.clip(1.0 + 0.18 * jax.random.normal(key_of[21], (D,), jnp.float32), 0.1, 1.9),
    }


RESIDUAL_SCALE = 2.0 ** 0.25
NORM_EPSILON = 1e-05
MIXER_EPSILON = 1e-06

def conv_silu(current, earlier, kernel):
    stacked = jnp.concatenate([earlier, current[:, None, :]], 1).astype(jnp.float32)
    return jax.nn.silu(lax.optimization_barrier(jnp.sum(stacked * kernel.astype(jnp.float32)[None], 1)))

def mixer_step(gate, values, writes, reads, steps, value_taps, write_taps, read_taps, past_values, past_writes, past_reads, step_bias, decay_log, skip_scale, state_past, mixer_gain):
    seq_count = gate.shape[0]
    values_act = conv_silu(values, past_values, value_taps).reshape(seq_count, HEADS, HEAD_DIM)
    writes_act = conv_silu(writes, past_writes, write_taps).reshape(seq_count, GROUPS, STATE_DIM)
    reads_act = conv_silu(reads, past_reads, read_taps).reshape(seq_count, GROUPS, STATE_DIM)
    per_group = HEADS // GROUPS
    writes_head = jnp.repeat(writes_act, per_group, axis=1)
    reads_head = jnp.repeat(reads_act, per_group, axis=1)
    step_size = jax.nn.softplus(steps.astype(jnp.float32) + step_bias)
    decays = jnp.exp(-step_size * jnp.exp(decay_log))
    state_next = decays[:, :, None, None] * state_past + (step_size[:, :, None] * values_act)[:, :, :, None] * writes_head[:, :, None, :]
    readout = jnp.einsum('shpn,shn->shp', state_next, reads_head, precision=lax.Precision.HIGHEST)
    readout = readout + skip_scale[None, :, None] * values_act
    gated = readout.reshape(seq_count, HEADS * HEAD_DIM) * jax.nn.silu(gate.astype(jnp.float32))
    grouped = gated.reshape(seq_count, GROUPS, -1)
    grouped = grouped * lax.rsqrt(lax.optimization_barrier(jnp.mean(jnp.square(grouped), -1, keepdims=True)) + MIXER_EPSILON)
    mixed = (grouped.reshape(seq_count, -1) * mixer_gain).astype(jnp.bfloat16)
    return (mixed, state_next)

def layer_norm(rows, gain):
    average = lax.optimization_barrier(jnp.mean(rows, -1, keepdims=True))
    variance = lax.optimization_barrier(jnp.mean(jnp.square(rows - average), -1, keepdims=True))
    return (rows - average) * lax.rsqrt(variance + NORM_EPSILON) * gain

def reference(layer_input, gate_weight, value_weight, write_weight, read_weight, step_weight, value_taps, write_taps, read_taps, past_values, past_writes, past_reads, step_bias, decay_log, skip_scale, state_past, mixer_gain, out_weight, norm1_gain, up_weight, down_weight, norm2_gain):

    def project(weight):
        return jnp.dot(layer_input, weight, preferred_element_type=jnp.float32).astype(jnp.bfloat16)
    gate = project(gate_weight)
    values = project(value_weight)
    writes = project(write_weight)
    reads = project(read_weight)
    steps = project(step_weight)
    mixed, state_next = mixer_step(gate, values, writes, reads, steps, value_taps, write_taps, read_taps, past_values, past_writes, past_reads, step_bias, decay_log, skip_scale, state_past, mixer_gain)
    mix_out = jnp.dot(mixed, out_weight, preferred_element_type=jnp.float32).astype(jnp.bfloat16)
    residual = RESIDUAL_SCALE * layer_input.astype(jnp.float32) + mix_out.astype(jnp.float32)
    normed = layer_norm(residual, norm1_gain).astype(jnp.bfloat16)
    hidden = jnp.square(jax.nn.relu(jnp.dot(normed, up_weight, preferred_element_type=jnp.float32))).astype(jnp.bfloat16)
    channel = jnp.dot(hidden, down_weight, preferred_element_type=jnp.float32).astype(jnp.bfloat16)
    second = RESIDUAL_SCALE * normed.astype(jnp.float32) + channel.astype(jnp.float32)
    layer_output = layer_norm(second, norm2_gain).astype(jnp.bfloat16)
    return (layer_output, state_next)
```

```python
import jax
import jax.numpy as jnp
from jax import lax
from jax.sharding import PartitionSpec as P

HEADS = 32
HEAD_DIM = 64
STATE_DIM = 128
GROUPS = 2
RESIDUAL_SCALE = 2.0**0.25
NORM_EPSILON = 1e-05
MIXER_EPSILON = 1e-06
SWAP = [(0, 1), (1, 0)]


def other_core(value):
    return lax.ppermute(value, "tp", SWAP)


def exchange(parts, axis):
    return lax.all_to_all(parts, axis, split_axis=0, concat_axis=0, tiled=True)


def copies_from(value, axis):
    return exchange(jnp.broadcast_to(value, (lax.axis_size(axis), *value.shape)), axis)


def conv_silu(current, earlier, kernel):
    stacked = jnp.concatenate([earlier, current[:, None, :]], 1).astype(jnp.float32)
    return jax.nn.silu(jnp.sum(stacked * kernel.astype(jnp.float32)[None], 1))


def mixer_step(
    gate,
    values,
    writes,
    reads,
    steps,
    value_taps,
    write_taps,
    read_taps,
    past_values,
    past_writes,
    past_reads,
    step_bias,
    decay_log,
    skip_scale,
    state_past,
    mixer_gain,
):
    seq_count = gate.shape[0]
    values_act = conv_silu(values, past_values, value_taps).reshape(seq_count, HEADS, HEAD_DIM)
    writes_act = conv_silu(writes, past_writes, write_taps).reshape(seq_count, GROUPS, STATE_DIM)
    reads_act = conv_silu(reads, past_reads, read_taps).reshape(seq_count, GROUPS, STATE_DIM)
    per_group = HEADS // GROUPS
    writes_head = jnp.repeat(writes_act, per_group, axis=1)
    reads_head = jnp.repeat(reads_act, per_group, axis=1)
    step_size = jax.nn.softplus(steps.astype(jnp.float32) + step_bias)
    decays = jnp.exp(-step_size * jnp.exp(decay_log))
    state_next = (
        decays[:, :, None, None] * state_past
        + (step_size[:, :, None] * values_act)[:, :, :, None] * writes_head[:, :, None, :]
    )
    readout = jnp.sum(state_next * reads_head[:, :, None, :], -1)
    readout = readout + skip_scale[None, :, None] * values_act
    gated = readout.reshape(seq_count, HEADS * HEAD_DIM) * jax.nn.silu(gate.astype(jnp.float32))
    grouped = gated.reshape(seq_count, GROUPS, -1)
    grouped = grouped * lax.rsqrt(jnp.mean(jnp.square(grouped), -1, keepdims=True) + MIXER_EPSILON)
    mixed = (grouped.reshape(seq_count, -1) * mixer_gain).astype(jnp.bfloat16)
    return (mixed, state_next)


def layer_norm(rows, gain):
    average = jnp.mean(rows, -1, keepdims=True)
    variance = jnp.mean(jnp.square(rows - average), -1, keepdims=True)
    return (rows - average) * lax.rsqrt(variance + NORM_EPSILON) * gain


def on_device(
    layer_input,
    gate_weight,
    value_weight,
    write_weight,
    read_weight,
    step_weight,
    value_taps,
    write_taps,
    read_taps,
    past_values,
    past_writes,
    past_reads,
    step_bias,
    decay_log,
    skip_scale,
    state_past,
    mixer_gain,
    out_weight,
    norm1_gain,
    up_weight,
    down_weight,
    norm2_gain,
):
    core = lax.axis_index("tp")
    chip = lax.axis_index("kv")
    chips = lax.axis_size("kv")
    width = norm1_gain.shape[0]
    rows = layer_input.shape[0] // (2 * chips)
    half = chips * rows
    weights = (gate_weight, value_weight, write_weight, read_weight, step_weight)

    input_rows = layer_input.reshape(chips, 2, rows, -1)
    own_input = lax.dynamic_index_in_dim(input_rows, core, 1, False).reshape(half, -1)
    far_input = lax.dynamic_index_in_dim(input_rows, 1 - core, 1, False).reshape(half, -1)

    def input_terms(of_rows):
        pieces = [jnp.dot(of_rows, weight, preferred_element_type=jnp.float32) for weight in weights]
        return jnp.concatenate(pieces, 1)

    arrived = other_core(input_terms(far_input).astype(jnp.bfloat16))
    terms = (input_terms(own_input) + arrived.astype(jnp.float32)).astype(jnp.bfloat16)
    projected = exchange(terms.reshape(chips, rows, -1), "kv").astype(jnp.float32).sum(0)
    projected = projected.astype(jnp.bfloat16)
    bounds = [0]
    for weight in weights:
        bounds.append(bounds[-1] + weight.shape[1])
    gate, values, writes, reads, steps = [
        projected[:, bounds[index] : bounds[index + 1]] for index in range(5)
    ]
    mixed, state_next = mixer_step(
        gate,
        values,
        writes,
        reads,
        steps,
        value_taps,
        write_taps,
        read_taps,
        past_values,
        past_writes,
        past_reads,
        step_bias,
        decay_log,
        skip_scale,
        state_past,
        mixer_gain,
    )
    own_mixed = copies_from(mixed, "kv").reshape(half, -1)
    far_mixed = other_core(own_mixed)

    def residual_of(mixed_rows, input_of_rows):
        mix_out = jnp.dot(mixed_rows, out_weight, preferred_element_type=jnp.float32)
        return (RESIDUAL_SCALE * input_of_rows.astype(jnp.float32) + mix_out).astype(jnp.bfloat16)

    def in_order(own, far, dim):
        first = jnp.where(core == 0, own, far)
        second = jnp.where(core == 0, far, own)
        return jnp.stack([first, second], dim)

    residual = in_order(residual_of(own_mixed, own_input), residual_of(far_mixed, far_input), 0)
    residual = residual.reshape(2 * half, -1)
    own_columns = copies_from(residual, "kv")
    far_columns = other_core(own_columns)
    whole = in_order(own_columns, far_columns, 1)
    whole = jnp.moveaxis(whole, 2, 0).reshape(2 * half, width).astype(jnp.float32)
    normed = layer_norm(whole, norm1_gain).astype(jnp.bfloat16)
    hidden = jnp.square(
        jax.nn.relu(jnp.dot(normed, up_weight, preferred_element_type=jnp.float32))
    ).astype(jnp.bfloat16)
    channel_terms = jnp.dot(hidden, down_weight, preferred_element_type=jnp.float32)
    own_terms = lax.dynamic_slice_in_dim(channel_terms, core * half, half, 0)
    far_terms = lax.dynamic_slice_in_dim(channel_terms, (1 - core) * half, half, 0)
    arrived = other_core(far_terms.astype(jnp.bfloat16))
    terms = (own_terms + arrived.astype(jnp.float32)).astype(jnp.bfloat16)
    channel = exchange(terms.reshape(chips, rows, width), "kv").astype(jnp.float32).sum(0)
    normed_own = lax.dynamic_slice_in_dim(normed, core * half + chip * rows, rows, 0)
    second = RESIDUAL_SCALE * normed_own.astype(jnp.float32) + channel
    result = layer_norm(second, norm2_gain).astype(jnp.bfloat16)
    result = jnp.moveaxis(result.reshape(rows, 2 * chips, -1), 1, 0)
    result = exchange(result, ("kv", "tp")).reshape(2 * half, -1)
    return (result, state_next)


def solution(mesh):
    placed = (
        P("dp", ("kv", "tp")),
        P(("kv", "tp"), None),
        P(("kv", "tp"), None),
        P(("kv", "tp"), None),
        P(("kv", "tp"), None),
        P(("kv", "tp"), None),
        P(),
        P(),
        P(),
        P(("dp", "kv", "tp"), None, None),
        P(("dp", "kv", "tp"), None, None),
        P(("dp", "kv", "tp"), None, None),
        P(),
        P(),
        P(),
        P(("dp", "kv", "tp"), None, None, None),
        P(),
        P(None, ("kv", "tp")),
        P(),
        P(None, ("kv", "tp")),
        P(("kv", "tp"), None),
        P(),
    )
    return jax.shard_map(
        on_device,
        mesh=mesh,
        in_specs=placed,
        out_specs=(P("dp", ("kv", "tp")), P(("dp", "kv", "tp"), None, None, None)),
        check_vma=False,
    )
```

```python
import jax
import jax.numpy as jnp
from jax import lax
from jax.experimental import pallas as pl
from jax.experimental.pallas import tpu as pltpu
from jax.sharding import PartitionSpec as P

HEADS = 32
HEAD_DIM = 64
STATE_DIM = 128
GROUPS = 2
RESIDUAL_SCALE = 2.0**0.25
NORM_EPSILON = 1e-05
MIXER_EPSILON = 1e-06
SWAP = [(0, 1), (1, 0)]
LANES = 128
F32 = jnp.float32
BF16 = jnp.bfloat16
NT = (((1,), (1,)), ((), ()))


def other_core(value):
    return lax.ppermute(value, "tp", SWAP)


def exchange(parts, axis):
    return lax.all_to_all(parts, axis, split_axis=0, concat_axis=0, tiled=True)


def kernel(body, outs, args, out_space=pltpu.VMEM, in_spaces=None, scratch=(), flops=0, limit=24):
    in_spaces = in_spaces or [pltpu.VMEM] * len(args)
    return pl.pallas_call(
        body,
        name=body.__name__,
        in_specs=[pl.BlockSpec(memory_space=space) for space in in_spaces],
        out_specs=[pl.BlockSpec(memory_space=out_space)] * len(outs),
        out_shape=[out_space(shape, dtype) for shape, dtype in outs],
        scratch_shapes=list(scratch),
        compiler_params=pltpu.CompilerParams(vmem_limit_bytes=limit * 2**20),
        cost_estimate=pl.CostEstimate(flops=flops, bytes_accessed=0, transcendentals=0),
    )(*[pltpu.with_memory_space_constraint(a, s) for a, s in zip(args, in_spaces)])


def dot(a, b):
    return jnp.dot(a, b, preferred_element_type=F32)


def sigmoid(value):
    return 1.0 / (1.0 + jnp.exp(-value))


def upper_rows(shape):
    return lax.broadcasted_iota(jnp.int32, shape, 0) % 8 < 4


def total_of(ref):
    total = ref[0].astype(F32)
    for j in range(1, ref.shape[0]):
        total = total + ref[j].astype(F32)
    return total


def project_rows(
    x_hbm,
    gate_hbm,
    value_hbm,
    write_hbm,
    read_hbm,
    step_hbm,
    far_ref,
    own_ref,
    order_ref,
    x_ref,
    gate_ref,
    value_ref,
    write_ref,
    read_ref,
    step_ref,
    rows_ref,
    arrivals,
):
    core = lax.axis_index("tp")
    pairs = (
        (x_hbm, x_ref),
        (step_hbm, step_ref.at[pl.ds(0, step_hbm.shape[0])]),
        (write_hbm, write_ref),
        (read_hbm, read_ref),
        (gate_hbm, gate_ref),
        (value_hbm, value_ref),
    )
    copies = [
        pltpu.make_async_copy(src, dst, arrivals.at[n]) for n, (src, dst) in enumerate(pairs)
    ]
    for copy in copies:
        copy.start()
    copies[0].wait()
    rows_ref[0] = x_ref[...].astype(F32)
    half = order_ref.shape[0] // 2
    for k in range(x_ref.shape[0] // 8):
        for c in range(2):
            order_ref[c * half + 4 * k : c * half + 4 * k + 4, :] = (
                RESIDUAL_SCALE * rows_ref[0, 8 * k + 4 * c : 8 * k + 4 * c + 4, :]
            )
        own = rows_ref[0, pl.ds(8 * k + 4 * core, 4), :]
        far = rows_ref[0, pl.ds(8 * k + 4 * (1 - core), 4), :]
        for place, value in ((1, own), (2, far)):
            rows_ref[place, pl.ds(8 * k, 4), :] = value
            rows_ref[place, pl.ds(8 * k + 4, 4), :] = value
    own = rows_ref[1].astype(BF16)
    far = rows_ref[2].astype(BF16)
    copies[1].wait()
    step_ref[step_hbm.shape[0] :, :] = jnp.zeros(
        (step_ref.shape[0] - step_hbm.shape[0], step_ref.shape[1]), BF16
    )
    inner, group = gate_ref.shape[1], write_ref.shape[1]
    for rows, out_ref in ((far, far_ref), (own, own_ref)):
        steps = lax.dot_general(rows, step_ref[...], NT, preferred_element_type=F32)
        steps = jnp.where(upper_rows(steps.shape), steps, 0.0)
        out_ref[:, :, inner + group :] = steps.astype(out_ref.dtype).reshape(-1, 8, LANES)
    copies[2].wait()
    copies[3].wait()
    for rows, out_ref in ((far, far_ref), (own, own_ref)):
        first, second = dot(rows, write_ref[...]), dot(rows, read_ref[...])
        both = jnp.where(upper_rows(first.shape), first, second).astype(out_ref.dtype)
        out_ref[:, :, inner : inner + group] = both.reshape(-1, 8, group)
    copies[4].wait()
    copies[5].wait()
    chunk = 512
    for rows, out_ref in ((far, far_ref), (own, own_ref)):
        for n in range(inner // chunk):
            at = slice(n * chunk, (n + 1) * chunk)
            first, second = dot(rows, gate_ref[:, at]), dot(rows, value_ref[:, at])
            both = jnp.where(upper_rows(first.shape), first, second).astype(out_ref.dtype)
            out_ref[:, :, at] = both.reshape(-1, 8, chunk)


def add_terms(own_ref, arrived_ref, *rest):
    out_ref = rest[-1]
    for k in range(out_ref.shape[0]):
        out_ref[k] = (own_ref[k] + arrived_ref[k].astype(F32)).astype(BF16)


def spread_heads(rows, inner):
    shape = (rows.shape[1], inner)
    spread = lax.broadcasted_iota(jnp.int32, shape, 1) // HEAD_DIM == lax.broadcasted_iota(
        jnp.int32, shape, 0
    )
    return dot(rows, spread.astype(F32).astype(BF16))


def prepare(
    state_hbm,
    past_value_hbm,
    past_write_hbm,
    past_read_hbm,
    value_taps_hbm,
    write_taps_hbm,
    read_taps_hbm,
    bias_hbm,
    rate_hbm,
    skip_hbm,
    state_ref,
    past_ref,
    taps_ref,
    head_ref,
    states_ref,
    past_value_ref,
    past_write_ref,
    past_read_ref,
    value_taps_ref,
    write_taps_ref,
    read_taps_ref,
    bias_ref,
    rate_ref,
    skip_ref,
    arrivals,
    state_arrivals,
):
    pairs = (
        (past_value_hbm, past_value_ref),
        (past_write_hbm, past_write_ref),
        (past_read_hbm, past_read_ref),
        (value_taps_hbm, value_taps_ref),
        (write_taps_hbm, write_taps_ref),
        (read_taps_hbm, read_taps_ref),
        (bias_hbm, bias_ref),
        (rate_hbm, rate_ref),
        (skip_hbm, skip_ref),
    )
    copies = [
        pltpu.make_async_copy(src, dst, arrivals.at[n]) for n, (src, dst) in enumerate(pairs)
    ]
    for copy in copies:
        copy.start()
    pieces = state_arrivals.shape[0]
    rows = state_ref.shape[0] // pieces
    state_copies = []
    for n in range(pieces):
        at = pl.ds(n * rows, rows)
        state_copies.append(
            pltpu.make_async_copy(state_hbm.at[at], states_ref.at[at], state_arrivals.at[n])
        )
        state_copies[-1].start()
    for copy in copies:
        copy.wait()
    at = 0
    for old_ref, tap_ref in (
        (past_value_ref, value_taps_ref),
        (past_write_ref, write_taps_ref),
        (past_read_ref, read_taps_ref),
    ):
        width = tap_ref.shape[1]
        taps = tap_ref[...].astype(F32)
        total = old_ref[0].astype(F32) * taps[0:1]
        for k in range(1, old_ref.shape[0]):
            total = total + old_ref[k].astype(F32) * taps[k : k + 1]
        past_ref[:, at : at + width] = total
        taps_ref[:, at : at + width] = taps[old_ref.shape[0] :]
        at += width
    heads = jnp.concatenate([bias_ref[...], jnp.exp(rate_ref[...]), skip_ref[...]], 0)
    terms = jnp.concatenate(split_terms(heads, 3), 0).astype(BF16)
    wide = spread_heads(terms, head_ref.shape[1])
    head_ref[...] = wide[0:3] + wide[3:6] + wide[6:9]
    for n in range(pieces):
        state_copies[n].wait()
        at = slice(n * rows, (n + 1) * rows)
        state_ref[at, :] = states_ref[at, :].astype(BF16)


def fetch(after_ref, up_hbm, up_ref, arrivals):
    pieces = arrivals.shape[0]
    rows = up_hbm.shape[0] // pieces
    copies = []
    for n in range(pieces):
        at = pl.ds(n * rows, rows)
        copies.append(pltpu.make_async_copy(up_hbm.at[at], up_ref.at[at], arrivals.at[n]))
        copies[-1].start()
    for copy in copies:
        copy.wait()


def mix(
    arrived_ref, past_ref, taps_ref, head_ref, gain_ref, state_ref, out_ref, decay_ref, drive_ref, write_ref
):
    inner = gain_ref.shape[1]
    seqs = out_ref.shape[1]
    group = inner // GROUPS
    span = GROUPS * STATE_DIM
    total = total_of(arrived_ref).astype(BF16).astype(F32)
    gate = total[:seqs, :inner]
    steps = total[:seqs, inner + span : inner + span + HEADS].astype(BF16)

    def active(new, at):
        conv = past_ref[:, at] + taps_ref[:, at] * new
        return conv * sigmoid(conv)

    values = active(total[seqs:, :inner], slice(0, inner))
    writes = active(total[:seqs, inner : inner + span], slice(inner, inner + span))
    reads = active(total[seqs:, inner : inner + span], slice(inner + span, inner + 2 * span))
    raw = spread_heads(steps, inner) + head_ref[0:1, :]
    step_size = jnp.maximum(raw, 0.0) + jnp.log1p(jnp.exp(-jnp.abs(raw)))
    decay = jnp.exp(-step_size * head_ref[1:2, :])
    drive = step_size * values
    high = reads.astype(BF16).astype(F32)
    low = reads - high
    row = lax.broadcasted_iota(jnp.int32, (seqs, group), 0)
    recalled, overlap = [], []
    for g in range(GROUPS):
        at = slice(g * STATE_DIM, (g + 1) * STATE_DIM)
        query = jnp.concatenate([high[:, at], low[:, at]], 0).astype(BF16)
        part = jnp.zeros((seqs, group), F32)
        for s in range(seqs):
            base = (s * GROUPS + g) * group
            found = lax.dot_general(query, state_ref[base : base + group, :], NT, preferred_element_type=F32)
            part = jnp.where(row == s, found[:seqs] + found[seqs:], part)
        recalled.append(part)
        both = jnp.sum(writes[:, at] * reads[:, at], 1, keepdims=True)
        overlap.append(jnp.broadcast_to(both, (seqs, group)))
    readout = (
        decay * jnp.concatenate(recalled, 1)
        + drive * jnp.concatenate(overlap, 1)
        + head_ref[2:3, :] * values
    )
    gated = readout * (gate * sigmoid(gate))
    normed = []
    for g in range(GROUPS):
        cut = gated[:, g * group : (g + 1) * group]
        mean = jnp.sum(cut * cut, 1, keepdims=True) * (1.0 / group)
        normed.append(cut * lax.rsqrt(mean + MIXER_EPSILON))
    mixed = (jnp.concatenate(normed, 1) * gain_ref[...]).astype(BF16)
    for k in range(out_ref.shape[0]):
        out_ref[k] = mixed
    decay_ref[...] = decay
    drive_ref[...] = drive
    write_ref[...] = writes


def split_terms(value, count):
    terms = []
    for _ in range(count):
        terms.append(value.astype(BF16).astype(F32))
        value = value - terms[-1]
    return terms


def next_state(
    state_hbm, decay_ref, drive_ref, write_ref, out_hbm, state_ref, out_ref, arrivals, departures
):
    seqs, inner = decay_ref.shape
    group = inner // GROUPS
    copies, loads = [], []
    for n in range(seqs * GROUPS):
        span = pl.ds(n * group, group)
        loads.append(pltpu.make_async_copy(state_hbm.at[span], state_ref.at[span], arrivals.at[n]))
        loads[-1].start()
    for s in range(seqs):
        for g in range(GROUPS):
            at = slice(g * group, (g + 1) * group)
            decay = split_terms(decay_ref[s : s + 1, at], 3)
            drive = split_terms(drive_ref[s : s + 1, at], 2)
            write = split_terms(write_ref[s : s + 1, g * STATE_DIM : (g + 1) * STATE_DIM], 2)
            one = jnp.ones((1, STATE_DIM), F32)
            blank_left, blank_right = jnp.zeros((5, group), F32), jnp.zeros((5, STATE_DIM), F32)
            left = jnp.concatenate([*decay, blank_left], 0).T.astype(BF16)
            right = jnp.concatenate([one, one, one, blank_right], 0).astype(BF16)
            factor = dot(left, right)
            left = jnp.concatenate([drive[0], drive[1], drive[0], blank_left], 0).T.astype(BF16)
            right = jnp.concatenate([write[0], write[0], write[1], blank_right], 0).astype(BF16)
            added = dot(left, right)
            base = (s * GROUPS + g) * group
            rows = slice(base, base + group)
            loads[s * GROUPS + g].wait()
            out_ref[rows, :] = factor * state_ref[rows, :] + added
            span = pl.ds(base, group)
            copies.append(
                pltpu.make_async_copy(
                    out_ref.at[span], out_hbm.at[span], departures.at[len(copies)]
                )
            )
            copies[-1].start()
    for copy in copies:
        copy.wait()


def channel_mixer(
    own_ref,
    far_ref,
    gain_ref,
    up_ref,
    down_hbm,
    far_out_ref,
    own_out_ref,
    row_ref,
    normed_ref,
    down_ref,
    arrivals,
):
    pieces = arrivals.shape[0]
    span = down_hbm.shape[0] // pieces
    copies = []
    for n in range(pieces):
        at = pl.ds(n * span, span)
        copies.append(pltpu.make_async_copy(down_hbm.at[at], down_ref.at[at], arrivals.at[n]))
        copies[-1].start()
    core = lax.axis_index("tp")
    chip = lax.axis_index("kv")
    chips, rows_all, lanes = own_ref.shape
    half = rows_all // 2
    width = 2 * chips * lanes
    total = jnp.zeros((rows_all, lanes), F32)
    for k in range(chips):
        total = total + own_ref[k].astype(F32) + far_ref[k].astype(F32)
    mean = jnp.sum(total, 1, keepdims=True) * (1.0 / width)
    square = jnp.zeros((rows_all, lanes), F32)
    for k in range(chips):
        a = own_ref[k].astype(F32) - mean
        b = far_ref[k].astype(F32) - mean
        square = square + a * a + b * b
    scale = lax.rsqrt(jnp.sum(square, 1, keepdims=True) * (1.0 / width) + NORM_EPSILON)
    for k in range(chips):
        own = own_ref[k].astype(F32)
        far = far_ref[k].astype(F32)
        pair = (jnp.where(core == 0, own, far), jnp.where(core == 0, far, own))
        for c in range(2):
            at = slice((2 * k + c) * lanes, (2 * k + c + 1) * lanes)
            normed_ref[:, at] = ((pair[c] - mean) * scale * gain_ref[:, at]).astype(BF16)
    hidden = jnp.maximum(dot(normed_ref[...], up_ref[...]), 0.0)
    hidden = (hidden * hidden).astype(BF16)
    for copy in copies:
        copy.wait()
    chunk = 256
    upper = upper_rows((half, chunk))
    for n in range(width // 2 // chunk):
        at = slice(n * chunk, (n + 1) * chunk)
        first = dot(hidden, down_ref[:, at])
        second = dot(hidden, down_ref[:, width // 2 + n * chunk : width // 2 + (n + 1) * chunk])
        for out_ref, here in ((far_out_ref, core == 1), (own_out_ref, core == 0)):
            a = jnp.where(here, first[:half], first[half:])
            b = jnp.where(here, second[:half], second[half:])
            even = jnp.where(upper, a, pltpu.roll(b, 4, 0)).astype(out_ref.dtype)
            odd = jnp.where(upper, pltpu.roll(a, half - 4, 0), b).astype(out_ref.dtype)
            for r in range(half // 8):
                out_ref[2 * r, :, at] = even[8 * r : 8 * r + 8]
                out_ref[2 * r + 1, :, at] = odd[8 * r : 8 * r + 8]
    shape = (8, rows_all)
    wanted = core * half + chip * 4 + lax.broadcasted_iota(jnp.int32, shape, 0) % 4
    pick = wanted == lax.broadcasted_iota(jnp.int32, shape, 1)
    rows = dot(pick.astype(F32).astype(BF16), normed_ref[...])
    row_ref[...] = jnp.where(
        upper_rows(row_ref.shape), rows[:, : width // 2], rows[:, width // 2 :]
    )


def last_norm(arrived_ref, row_ref, gain_ref, out_ref):
    second = RESIDUAL_SCALE * row_ref[...] + total_of(arrived_ref)
    half = second.shape[1]

    def row_mean(value):
        sums = jnp.broadcast_to(jnp.sum(value, 1, keepdims=True), (8, LANES))
        sums = (sums + pltpu.roll(sums, 4, 0)) * (0.5 / half)
        return sums[:, 0:1]

    centred = second - row_mean(second)
    scale = lax.rsqrt(row_mean(centred * centred) + NORM_EPSILON)
    gain = jnp.where(upper_rows(second.shape), gain_ref[:, :half], gain_ref[:, half:])
    result = centred * scale * gain
    for j in range(half // LANES):
        both = result[:, j * LANES : (j + 1) * LANES]
        out_ref[j] = both[:4].astype(BF16)
        out_ref[half // LANES + j] = both[4:].astype(BF16)


def on_device(
    layer_input,
    gate_weight,
    value_weight,
    write_weight,
    read_weight,
    step_weight,
    value_taps,
    write_taps,
    read_taps,
    past_values,
    past_writes,
    past_reads,
    step_bias,
    decay_log,
    skip_scale,
    state_past,
    mixer_gain,
    out_weight,
    norm1_gain,
    up_weight,
    down_weight,
    norm2_gain,
):
    core = lax.axis_index("tp")
    chips = lax.axis_size("kv")
    width = norm1_gain.shape[0]
    inner = mixer_gain.shape[0]
    rows = layer_input.shape[0] // (2 * chips)
    half = chips * rows
    per_head = inner // HEADS

    span = GROUPS * STATE_DIM
    terms_width = inner + span + LANES
    far_terms, own_terms, scaled_input = kernel(
        project_rows,
        [((chips, 8, terms_width), BF16), ((chips, 8, terms_width), F32), (layer_input.shape, F32)],
        [layer_input, gate_weight, value_weight, write_weight, read_weight, step_weight.T],
        in_spaces=[pltpu.HBM] * 6,
        scratch=[
            pltpu.VMEM(layer_input.shape, BF16),
            pltpu.VMEM(gate_weight.shape, BF16),
            pltpu.VMEM(value_weight.shape, BF16),
            pltpu.VMEM(write_weight.shape, BF16),
            pltpu.VMEM(read_weight.shape, BF16),
            pltpu.VMEM((LANES, LANES), BF16),
            pltpu.VMEM((3, 2 * half, LANES), F32),
            pltpu.SemaphoreType.DMA((6,)),
        ],
        flops=2**28,
    )
    arrived = other_core(far_terms)
    state_rows = state_past.reshape(-1, STATE_DIM)
    small = [jnp.swapaxes(p, 0, 1) for p in (past_values, past_writes, past_reads)]
    small += [value_taps, write_taps, read_taps]
    small += [step_bias[None], decay_log[None], skip_scale[None]]
    conv_width = inner + 2 * span
    states, past, taps, heads = kernel(
        prepare,
        [
            (state_rows.shape, BF16),
            ((rows, conv_width), F32),
            ((1, conv_width), F32),
            ((3, inner), F32),
        ],
        [state_rows, *small],
        in_spaces=[pltpu.HBM] * 10,
        scratch=[
            pltpu.VMEM(state_rows.shape, F32),
            *[pltpu.VMEM(a.shape, a.dtype) for a in small],
            pltpu.SemaphoreType.DMA((9,)),
            pltpu.SemaphoreType.DMA((8,)),
        ],
        flops=2**29,
    )
    (terms,) = kernel(
        add_terms, [((chips, 8, terms_width), BF16)], [own_terms, arrived, taps], flops=2**20
    )
    arrived = exchange(terms, "kv")
    mixed, decay, drive, writes = kernel(
        mix,
        [
            ((chips, rows, inner), BF16),
            ((rows, inner), F32),
            ((rows, inner), F32),
            ((rows, span), F32),
        ],
        [arrived, past, taps, heads, mixer_gain[None], states],
        flops=2**28,
    )
    own_mixed = exchange(mixed, "kv").reshape(half, inner)
    far_mixed = other_core(own_mixed)

    (state_next,) = kernel(
        next_state,
        [(state_rows.shape, F32)],
        [state_rows, decay, drive, writes],
        in_spaces=[pltpu.HBM] + [pltpu.VMEM] * 3,
        out_space=pltpu.HBM,
        scratch=[
            pltpu.VMEM(state_rows.shape, F32),
            pltpu.VMEM(state_rows.shape, F32),
            pltpu.SemaphoreType.DMA((8,)),
            pltpu.SemaphoreType.DMA((8,)),
        ],
        flops=2**30,
    )
    state_next = state_next.reshape(state_past.shape)

    own_mix, far_mix = dot(own_mixed, out_weight), dot(far_mixed, out_weight)
    mix_out = jnp.concatenate(
        [jnp.where(core == 0, own_mix, far_mix), jnp.where(core == 0, far_mix, own_mix)], 0
    )
    residual = (scaled_input + mix_out).astype(BF16)
    own_columns = exchange(jnp.broadcast_to(residual, (chips, *residual.shape)), "kv")
    far_columns = other_core(own_columns)
    (up_here,) = kernel(
        fetch,
        [(up_weight.shape, BF16)],
        [own_columns, up_weight],
        in_spaces=[pltpu.VMEM, pltpu.HBM],
        scratch=[pltpu.SemaphoreType.DMA((8,))],
        flops=2**30,
        limit=4,
    )
    far_terms, own_terms, normed_rows = kernel(
        channel_mixer,
        [((chips, 8, width // 2), BF16), ((chips, 8, width // 2), F32), ((8, width // 2), F32)],
        [own_columns, far_columns, norm1_gain[None], up_here, down_weight],
        in_spaces=[pltpu.VMEM] * 4 + [pltpu.HBM],
        scratch=[
            pltpu.VMEM((2 * half, width), BF16),
            pltpu.VMEM(down_weight.shape, BF16),
            pltpu.SemaphoreType.DMA((4,)),
        ],
        flops=2**30,
    )
    arrived = other_core(far_terms)
    (terms,) = kernel(
        add_terms, [((chips, 8, width // 2), BF16)], [own_terms, arrived], flops=2**20
    )
    arrived = exchange(terms, "kv")
    (result,) = kernel(
        last_norm,
        [((2 * chips, rows, LANES), BF16)],
        [arrived, normed_rows, norm2_gain[None]],
        flops=2**20,
    )
    result = exchange(result, ("kv", "tp")).reshape(2 * half, LANES)
    return (result, state_next)


def solution(mesh):
    placed = (
        P("dp", ("kv", "tp")),
        P(("kv", "tp"), None),
        P(("kv", "tp"), None),
        P(("kv", "tp"), None),
        P(("kv", "tp"), None),
        P(("kv", "tp"), None),
        P(),
        P(),
        P(),
        P(("dp", "kv", "tp"), None, None),
        P(("dp", "kv", "tp"), None, None),
        P(("dp", "kv", "tp"), None, None),
        P(),
        P(),
        P(),
        P(("dp", "kv", "tp"), None, None, None),
        P(),
        P(None, ("kv", "tp")),
        P(),
        P(None, ("kv", "tp")),
        P(("kv", "tp"), None),
        P(),
    )
    return jax.shard_map(
        on_device,
        mesh=mesh,
        in_specs=placed,
        out_specs=(P("dp", ("kv", "tp")), P(("dp", "kv", "tp"), None, None, None)),
        check_vma=False,
    )
```

```python
import jax
import jax.numpy as jnp
from jax import lax
from jax.experimental import pallas as pl
from jax.experimental.pallas import tpu as pltpu
from jax.sharding import PartitionSpec as P

HEADS = 32
HEAD_DIM = 64
STATE_DIM = 128
GROUPS = 2
RESIDUAL_SCALE = 2.0**0.25
NORM_EPSILON = 1e-05
MIXER_EPSILON = 1e-06
SWAP = [(0, 1), (1, 0)]
LANES = 128
F32 = jnp.float32
BF16 = jnp.bfloat16
NT = (((1,), (1,)), ((), ()))


def other_core(value):
    return lax.ppermute(value, "tp", SWAP)


def exchange(parts, axis):
    return lax.all_to_all(parts, axis, split_axis=0, concat_axis=0, tiled=True)


def kernel(body, outs, args, out_space=pltpu.VMEM, in_spaces=None, scratch=(), flops=0, limit=12):
    in_spaces = in_spaces or [pltpu.VMEM] * len(args)
    return pl.pallas_call(
        body,
        name=body.__name__,
        in_specs=[pl.BlockSpec(memory_space=space) for space in in_spaces],
        out_specs=[pl.BlockSpec(memory_space=out_space)] * len(outs),
        out_shape=[out_space(shape, dtype) for shape, dtype in outs],
        scratch_shapes=list(scratch),
        compiler_params=pltpu.CompilerParams(vmem_limit_bytes=limit * 2**20),
        cost_estimate=pl.CostEstimate(flops=flops, bytes_accessed=0, transcendentals=0),
    )(*[pltpu.with_memory_space_constraint(a, s) for a, s in zip(args, in_spaces)])


def dot(a, b):
    return jnp.dot(a, b, preferred_element_type=F32)


def sigmoid(value):
    return lax.logistic(value)


def upper_rows(shape):
    return lax.broadcasted_iota(jnp.int32, shape, 0) % 8 < 4


def total_of(ref):
    total = ref[0].astype(F32)
    for j in range(1, ref.shape[0]):
        total = total + ref[j].astype(F32)
    return total


def project_rows(
    x_hbm,
    gate_hbm,
    value_hbm,
    write_hbm,
    read_hbm,
    step_hbm,
    far_ref,
    own_ref,
    x_ref,
    gate_ref,
    value_ref,
    write_ref,
    read_ref,
    step_ref,
    rows_ref,
    arrivals,
):
    core = lax.axis_index("tp")
    pairs = (
        (x_hbm, x_ref),
        (step_hbm, step_ref.at[pl.ds(0, step_hbm.shape[0])]),
        (write_hbm, write_ref),
        (read_hbm, read_ref),
        (gate_hbm, gate_ref),
        (value_hbm, value_ref),
    )
    copies = [
        pltpu.make_async_copy(src, dst, arrivals.at[n]) for n, (src, dst) in enumerate(pairs)
    ]
    for copy in copies:
        copy.start()
    copies[0].wait()
    rows_ref[0] = x_ref[...].astype(F32)
    for k in range(x_ref.shape[0] // 8):
        own = rows_ref[0, pl.ds(8 * k + 4 * core, 4), :]
        far = rows_ref[0, pl.ds(8 * k + 4 * (1 - core), 4), :]
        for place, value in ((1, own), (2, far)):
            rows_ref[place, pl.ds(8 * k, 4), :] = value
            rows_ref[place, pl.ds(8 * k + 4, 4), :] = value
    own = rows_ref[1].astype(BF16)
    far = rows_ref[2].astype(BF16)
    copies[1].wait()
    step_ref[step_hbm.shape[0] :, :] = jnp.zeros(
        (step_ref.shape[0] - step_hbm.shape[0], step_ref.shape[1]), BF16
    )
    inner, group = gate_ref.shape[1], write_ref.shape[1]
    for rows, out_ref in ((far, far_ref), (own, own_ref)):
        steps = lax.dot_general(rows, step_ref[...], NT, preferred_element_type=F32)
        steps = jnp.where(upper_rows(steps.shape), steps, 0.0)
        out_ref[:, :, inner + group :] = steps.astype(out_ref.dtype).reshape(-1, 8, LANES)
    copies[2].wait()
    copies[3].wait()
    for rows, out_ref in ((far, far_ref), (own, own_ref)):
        first, second = dot(rows, write_ref[...]), dot(rows, read_ref[...])
        both = jnp.where(upper_rows(first.shape), first, second).astype(out_ref.dtype)
        out_ref[:, :, inner : inner + group] = both.reshape(-1, 8, group)
    copies[4].wait()
    copies[5].wait()
    chunk = 512
    for rows, out_ref in ((far, far_ref), (own, own_ref)):
        for n in range(inner // chunk):
            at = slice(n * chunk, (n + 1) * chunk)
            first, second = dot(rows, gate_ref[:, at]), dot(rows, value_ref[:, at])
            both = jnp.where(upper_rows(first.shape), first, second).astype(out_ref.dtype)
            out_ref[:, :, at] = both.reshape(-1, 8, chunk)


def add_terms(own_ref, arrived_ref, *rest):
    out_ref = rest[-1]
    for k in range(out_ref.shape[0]):
        out_ref[k] = (own_ref[k] + arrived_ref[k].astype(F32)).astype(BF16)


def spread_heads(rows, inner):
    shape = (rows.shape[1], inner)
    spread = lax.broadcasted_iota(jnp.int32, shape, 1) // HEAD_DIM == lax.broadcasted_iota(
        jnp.int32, shape, 0
    )
    return dot(rows, spread.astype(F32).astype(BF16))


def prepare(
    state_hbm,
    past_value_hbm,
    past_write_hbm,
    past_read_hbm,
    value_taps_hbm,
    write_taps_hbm,
    read_taps_hbm,
    bias_hbm,
    rate_hbm,
    skip_hbm,
    state_ref,
    past_ref,
    taps_ref,
    head_ref,
    states_ref,
    past_value_ref,
    past_write_ref,
    past_read_ref,
    value_taps_ref,
    write_taps_ref,
    read_taps_ref,
    bias_ref,
    rate_ref,
    skip_ref,
    arrivals,
    state_arrivals,
):
    pairs = (
        (past_value_hbm, past_value_ref),
        (past_write_hbm, past_write_ref),
        (past_read_hbm, past_read_ref),
        (value_taps_hbm, value_taps_ref),
        (write_taps_hbm, write_taps_ref),
        (read_taps_hbm, read_taps_ref),
        (bias_hbm, bias_ref),
        (rate_hbm, rate_ref),
        (skip_hbm, skip_ref),
    )
    copies = [
        pltpu.make_async_copy(src, dst, arrivals.at[n]) for n, (src, dst) in enumerate(pairs)
    ]
    for copy in copies:
        copy.start()
    pieces = state_arrivals.shape[0]
    rows = state_ref.shape[0] // pieces
    state_copies = []
    for n in range(pieces):
        at = pl.ds(n * rows, rows)
        state_copies.append(
            pltpu.make_async_copy(state_hbm.at[at], states_ref.at[at], state_arrivals.at[n])
        )
        state_copies[-1].start()
    for copy in copies:
        copy.wait()
    at = 0
    for old_ref, tap_ref in (
        (past_value_ref, value_taps_ref),
        (past_write_ref, write_taps_ref),
        (past_read_ref, read_taps_ref),
    ):
        width = tap_ref.shape[1]
        taps = tap_ref[...].astype(F32)
        total = old_ref[0].astype(F32) * taps[0:1]
        for k in range(1, old_ref.shape[0]):
            total = total + old_ref[k].astype(F32) * taps[k : k + 1]
        past_ref[:, at : at + width] = total
        taps_ref[:, at : at + width] = taps[old_ref.shape[0] :]
        at += width
    heads = jnp.concatenate([bias_ref[...], jnp.exp(rate_ref[...]), skip_ref[...]], 0)
    terms = jnp.concatenate(split_terms(heads, 3), 0).astype(BF16)
    wide = spread_heads(terms, head_ref.shape[1])
    head_ref[...] = wide[0:3] + wide[3:6] + wide[6:9]
    for n in range(pieces):
        state_copies[n].wait()
        at = slice(n * rows, (n + 1) * rows)
        state_ref[at, :] = states_ref[at, :].astype(BF16)


def mix_out(mixed_ref, own_weight_ref, far_weight_ref, own_input_ref, far_input_ref, out_ref, rows_ref):
    core = lax.axis_index("tp")
    lanes = own_input_ref.shape[1]
    group = mixed_ref.shape[2]
    half = out_ref.shape[1]
    rows_ref[0] = own_input_ref[...].astype(F32)
    rows_ref[1] = far_input_ref[...].astype(F32)
    for k in range(half // 4):
        for n in range(2):
            rows_ref[2 + n, 4 * k : 4 * k + 4, :] = rows_ref[n, pl.ds(8 * k + 4 * core, 4), :]
    mixed = mixed_ref[...].reshape(2 * half, group)
    upper = upper_rows((half, lanes))
    parts = []
    for n, weight_ref in enumerate((own_weight_ref, far_weight_ref)):
        first = dot(mixed, weight_ref[:group, :])
        second = dot(mixed, weight_ref[group:, :])
        both = (first + pltpu.roll(second, 2 * half - 4, 0)).reshape(half // 8, 16, lanes)
        even = both[:, :8].reshape(half, lanes)
        odd = both[:, 8:].reshape(half, lanes)
        total = jnp.where(upper, even, pltpu.roll(odd, 4, 0))
        parts.append((RESIDUAL_SCALE * rows_ref[2 + n, :half] + total).astype(BF16))
    first = jnp.where(core == 0, parts[0], parts[1])
    second = jnp.where(core == 0, parts[1], parts[0])
    for k in range(out_ref.shape[0]):
        out_ref[k, :, :lanes] = first
        out_ref[k, :, lanes:] = second


def mix(
    arrived_ref,
    past_ref,
    taps_ref,
    head_ref,
    gain_ref,
    state_ref,
    out_ref,
    decay_ref,
    drive_ref,
    write_ref,
):
    inner = gain_ref.shape[1]
    seqs = out_ref.shape[1] // GROUPS
    group = inner // GROUPS
    span = GROUPS * STATE_DIM
    total = total_of(arrived_ref).astype(BF16).astype(F32)
    gate = total[:seqs, :inner]
    steps = total[:seqs, inner + span : inner + span + HEADS].astype(BF16)

    def active(new, at):
        conv = past_ref[:, at] + taps_ref[:, at] * new
        return conv * sigmoid(conv)

    values = active(total[seqs:, :inner], slice(0, inner))
    writes = active(total[:seqs, inner : inner + span], slice(inner, inner + span))
    reads = active(total[seqs:, inner : inner + span], slice(inner + span, inner + 2 * span))
    raw = spread_heads(steps, inner) + head_ref[0:1, :]
    step_size = jnp.maximum(raw, 0.0) + jnp.log1p(jnp.exp(-jnp.abs(raw)))
    decay = jnp.exp(-step_size * head_ref[1:2, :])
    drive = step_size * values
    high = reads.astype(BF16).astype(F32)
    low = reads - high
    row = lax.broadcasted_iota(jnp.int32, (seqs, group), 0)
    recalled, overlap = [], []
    for g in range(GROUPS):
        at = slice(g * STATE_DIM, (g + 1) * STATE_DIM)
        query = jnp.concatenate([high[:, at], low[:, at]], 0).astype(BF16)
        part = jnp.zeros((seqs, group), F32)
        for s in range(seqs):
            base = (s * GROUPS + g) * group
            found = lax.dot_general(query, state_ref[base : base + group, :], NT, preferred_element_type=F32)
            part = jnp.where(row == s, found[:seqs] + found[seqs:], part)
        recalled.append(part)
        both = jnp.sum(writes[:, at] * reads[:, at], 1, keepdims=True)
        overlap.append(jnp.broadcast_to(both, (seqs, group)))
    readout = (
        decay * jnp.concatenate(recalled, 1)
        + drive * jnp.concatenate(overlap, 1)
        + head_ref[2:3, :] * values
    )
    gated = readout * (gate * sigmoid(gate))
    normed = []
    for g in range(GROUPS):
        cut = gated[:, g * group : (g + 1) * group]
        mean = jnp.sum(cut * cut, 1, keepdims=True) * (1.0 / group)
        normed.append(cut * lax.rsqrt(mean + MIXER_EPSILON))
    mixed = [normed[g] * gain_ref[:, g * group : (g + 1) * group] for g in range(GROUPS)]
    mixed = jnp.concatenate(mixed, 0).astype(BF16)
    for k in range(out_ref.shape[0]):
        out_ref[k] = mixed
    decay_ref[...] = decay
    drive_ref[...] = drive
    write_ref[...] = writes


def split_terms(value, count):
    terms = []
    for _ in range(count):
        terms.append(value.astype(BF16).astype(F32))
        value = value - terms[-1]
    return terms


def next_state(
    state_hbm, decay_ref, drive_ref, write_ref, out_hbm, state_ref, out_ref, arrivals, departures
):
    seqs, inner = decay_ref.shape
    group = inner // GROUPS
    copies, loads = [], []
    for n in range(seqs * GROUPS):
        span = pl.ds(n * group, group)
        loads.append(pltpu.make_async_copy(state_hbm.at[span], state_ref.at[span], arrivals.at[n]))
        loads[-1].start()
    for s in range(seqs):
        for g in range(GROUPS):
            at = slice(g * group, (g + 1) * group)
            decay = split_terms(decay_ref[s : s + 1, at], 3)
            drive = split_terms(drive_ref[s : s + 1, at], 2)
            write = split_terms(write_ref[s : s + 1, g * STATE_DIM : (g + 1) * STATE_DIM], 2)
            one = jnp.ones((1, STATE_DIM), F32)
            blank_left, blank_right = jnp.zeros((5, group), F32), jnp.zeros((5, STATE_DIM), F32)
            left = jnp.concatenate([*decay, blank_left], 0).T.astype(BF16)
            right = jnp.concatenate([one, one, one, blank_right], 0).astype(BF16)
            factor = dot(left, right)
            left = jnp.concatenate([drive[0], drive[1], drive[0], blank_left], 0).T.astype(BF16)
            right = jnp.concatenate([write[0], write[0], write[1], blank_right], 0).astype(BF16)
            added = dot(left, right)
            base = (s * GROUPS + g) * group
            rows = slice(base, base + group)
            loads[s * GROUPS + g].wait()
            out_ref[rows, :] = factor * state_ref[rows, :] + added
            span = pl.ds(base, group)
            copies.append(
                pltpu.make_async_copy(
                    out_ref.at[span], out_hbm.at[span], departures.at[len(copies)]
                )
            )
            copies[-1].start()
    for copy in copies:
        copy.wait()


def channel_mixer(
    cols_ref,
    gain_ref,
    up_own_ref,
    up_far_ref,
    down_own_ref,
    down_far_ref,
    out_ref,
    row_ref,
    normed_ref,
):
    chip = lax.axis_index("kv")
    chips, half, lanes = cols_ref.shape
    width = chips * lanes
    total = jnp.zeros((half, lanes), F32)
    for k in range(chips):
        total = total + cols_ref[k].astype(F32)
    mean = jnp.sum(total, 1, keepdims=True) * (1.0 / width)
    square = jnp.zeros((half, lanes), F32)
    for k in range(chips):
        a = cols_ref[k].astype(F32) - mean
        square = square + a * a
    scale = lax.rsqrt(jnp.sum(square, 1, keepdims=True) * (1.0 / width) + NORM_EPSILON)
    for k in range(chips):
        at = slice(k * lanes, (k + 1) * lanes)
        centred = cols_ref[k].astype(F32) - mean
        normed_ref[:, at] = (centred * scale * gain_ref[:, at]).astype(BF16)
    hidden = []
    for weight_ref in (up_own_ref, up_far_ref):
        active = jnp.maximum(dot(normed_ref[...], weight_ref[...]), 0.0)
        hidden.append((active * active).astype(BF16))
    chunk = 256
    upper = upper_rows((half, chunk))
    for n in range(width // 2 // chunk):
        at = slice(n * chunk, (n + 1) * chunk)
        past = slice(width // 2 + n * chunk, width // 2 + (n + 1) * chunk)
        a = dot(hidden[0], down_own_ref[:, at]) + dot(hidden[1], down_far_ref[:, at])
        b = dot(hidden[0], down_own_ref[:, past]) + dot(hidden[1], down_far_ref[:, past])
        even = jnp.where(upper, a, pltpu.roll(b, 4, 0)).astype(out_ref.dtype)
        odd = jnp.where(upper, pltpu.roll(a, half - 4, 0), b).astype(out_ref.dtype)
        for r in range(half // 8):
            out_ref[2 * r, :, at] = even[8 * r : 8 * r + 8]
            out_ref[2 * r + 1, :, at] = odd[8 * r : 8 * r + 8]
    shape = (8, half)
    wanted = chip * 4 + lax.broadcasted_iota(jnp.int32, shape, 0) % 4
    pick = wanted == lax.broadcasted_iota(jnp.int32, shape, 1)
    rows = dot(pick.astype(F32).astype(BF16), normed_ref[...])
    row_ref[...] = jnp.where(
        upper_rows(row_ref.shape), rows[:, : width // 2], rows[:, width // 2 :]
    )


def last_norm(arrived_ref, row_ref, gain_ref, out_ref):
    second = RESIDUAL_SCALE * row_ref[...] + total_of(arrived_ref)
    half = second.shape[1]

    def row_mean(value):
        sums = jnp.broadcast_to(jnp.sum(value, 1, keepdims=True), (8, LANES))
        sums = (sums + pltpu.roll(sums, 4, 0)) * (0.5 / half)
        return sums[:, 0:1]

    centred = second - row_mean(second)
    scale = lax.rsqrt(row_mean(centred * centred) + NORM_EPSILON)
    gain = jnp.where(upper_rows(second.shape), gain_ref[:, :half], gain_ref[:, half:])
    result = centred * scale * gain
    for j in range(half // LANES):
        both = result[:, j * LANES : (j + 1) * LANES]
        out_ref[j] = both[:4].astype(BF16)
        out_ref[half // LANES + j] = both[4:].astype(BF16)


def on_device(
    layer_input,
    gate_weight,
    value_weight,
    write_weight,
    read_weight,
    step_weight,
    value_taps,
    write_taps,
    read_taps,
    past_values,
    past_writes,
    past_reads,
    step_bias,
    decay_log,
    skip_scale,
    state_past,
    mixer_gain,
    out_weight,
    norm1_gain,
    up_weight,
    down_weight,
    norm2_gain,
):
    chips = lax.axis_size("kv")
    width = norm1_gain.shape[0]
    inner = mixer_gain.shape[0]
    rows = layer_input.shape[0] // (2 * chips)
    half = chips * rows
    per_head = inner // HEADS

    span = GROUPS * STATE_DIM
    terms_width = inner + span + LANES
    far_terms, own_terms = kernel(
        project_rows,
        [((chips, 8, terms_width), BF16), ((chips, 8, terms_width), F32)],
        [layer_input, gate_weight, value_weight, write_weight, read_weight, step_weight.T],
        in_spaces=[pltpu.HBM] * 6,
        scratch=[
            pltpu.VMEM(layer_input.shape, BF16),
            pltpu.VMEM(gate_weight.shape, BF16),
            pltpu.VMEM(value_weight.shape, BF16),
            pltpu.VMEM(write_weight.shape, BF16),
            pltpu.VMEM(read_weight.shape, BF16),
            pltpu.VMEM((LANES, LANES), BF16),
            pltpu.VMEM((3, 2 * half, LANES), F32),
            pltpu.SemaphoreType.DMA((6,)),
        ],
        flops=2**28,
    )
    arrived = other_core(far_terms)
    state_rows = state_past.reshape(-1, STATE_DIM)
    small = [jnp.swapaxes(p, 0, 1) for p in (past_values, past_writes, past_reads)]
    small += [value_taps, write_taps, read_taps]
    small += [step_bias[None], decay_log[None], skip_scale[None]]
    conv_width = inner + 2 * span
    states, past, taps, heads = kernel(
        prepare,
        [
            (state_rows.shape, BF16),
            ((rows, conv_width), F32),
            ((1, conv_width), F32),
            ((3, inner), F32),
        ],
        [state_rows, *small],
        in_spaces=[pltpu.HBM] * 10,
        scratch=[
            pltpu.VMEM(state_rows.shape, F32),
            *[pltpu.VMEM(a.shape, a.dtype) for a in small],
            pltpu.SemaphoreType.DMA((9,)),
            pltpu.SemaphoreType.DMA((8,)),
        ],
        flops=2**29,
    )
    (terms,) = kernel(
        add_terms, [((chips, 8, terms_width), BF16)], [own_terms, arrived, taps], flops=2**20
    )
    terms, far_input, far_out, up_from, down_from = lax.optimization_barrier(
        (terms, other_core(layer_input), other_core(out_weight), up_weight, down_weight)
    )
    swapped = [other_core(weight) for weight in (up_from, down_from)]
    arrived = exchange(terms, "kv")
    arrived, far_up, far_down = lax.optimization_barrier((arrived, *swapped))
    mixed, decay, drive, writes = kernel(
        mix,
        [
            ((chips, GROUPS * rows, inner // GROUPS), BF16),
            ((rows, inner), F32),
            ((rows, inner), F32),
            ((rows, span), F32),
        ],
        [arrived, past, taps, heads, mixer_gain[None], states],
        flops=2**28,
    )
    mixed = exchange(mixed, "kv")

    (state_next,) = kernel(
        next_state,
        [(state_rows.shape, F32)],
        [state_rows, decay, drive, writes],
        in_spaces=[pltpu.HBM] + [pltpu.VMEM] * 3,
        out_space=pltpu.HBM,
        scratch=[
            pltpu.VMEM(state_rows.shape, F32),
            pltpu.VMEM(state_rows.shape, F32),
            pltpu.SemaphoreType.DMA((8,)),
            pltpu.SemaphoreType.DMA((8,)),
        ],
        flops=2**30,
    )
    state_next = state_next.reshape(state_past.shape)

    (columns,) = kernel(
        mix_out,
        [((chips, half, 2 * LANES), BF16)],
        [mixed, out_weight, far_out, layer_input, far_input],
        scratch=[pltpu.VMEM((4, 2 * half, LANES), F32)],
        flops=2**28,
    )
    columns = exchange(columns, "kv")
    terms, normed_rows = kernel(
        channel_mixer,
        [((chips, 8, width // 2), BF16), ((8, width // 2), F32)],
        [columns, norm1_gain[None], up_weight, far_up, down_weight, far_down],
        scratch=[pltpu.VMEM((half, width), BF16)],
        flops=2**31,
    )
    arrived = exchange(terms, "kv")
    (result,) = kernel(
        last_norm,
        [((2 * chips, rows, LANES), BF16)],
        [arrived, normed_rows, norm2_gain[None]],
        flops=2**20,
    )
    result = exchange(result, ("kv", "tp")).reshape(2 * half, LANES)
    return (result, state_next)


def solution(mesh):
    placed = (
        P("dp", ("kv", "tp")),
        P(("kv", "tp"), None),
        P(("kv", "tp"), None),
        P(("kv", "tp"), None),
        P(("kv", "tp"), None),
        P(("kv", "tp"), None),
        P(),
        P(),
        P(),
        P(("dp", "kv", "tp"), None, None),
        P(("dp", "kv", "tp"), None, None),
        P(("dp", "kv", "tp"), None, None),
        P(),
        P(),
        P(),
        P(("dp", "kv", "tp"), None, None, None),
        P(),
        P(None, ("kv", "tp")),
        P(),
        P(None, ("kv", "tp")),
        P(("kv", "tp"), None),
        P(),
    )
    return jax.shard_map(
        on_device,
        mesh=mesh,
        in_specs=placed,
        out_specs=(P("dp", ("kv", "tp")), P(("dp", "kv", "tp"), None, None, None)),
        check_vma=False,
    )
```

```python
import jax
import jax.numpy as jnp
from jax import lax
from jax.experimental import pallas as pl
from jax.experimental.pallas import tpu as pltpu
from jax.sharding import PartitionSpec as P

HEADS = 32
HEAD_DIM = 64
STATE_DIM = 128
GROUPS = 2
RESIDUAL_SCALE = 2.0**0.25
NORM_EPSILON = 1e-05
MIXER_EPSILON = 1e-06
SWAP = [(0, 1), (1, 0)]
LANES = 128
F32 = jnp.float32
BF16 = jnp.bfloat16
NT = (((1,), (1,)), ((), ()))


def other_core(value):
    return lax.ppermute(value, "tp", SWAP)


def exchange(parts, axis):
    return lax.all_to_all(parts, axis, split_axis=0, concat_axis=0, tiled=True)


def kernel(body, outs, args, out_spaces=None, in_spaces=None, scratch=(), flops=0, limit=12):
    in_spaces = in_spaces or [pltpu.VMEM] * len(args)
    out_spaces = out_spaces or [pltpu.VMEM] * len(outs)
    return pl.pallas_call(
        body,
        name=body.__name__,
        in_specs=[pl.BlockSpec(memory_space=space) for space in in_spaces],
        out_specs=[pl.BlockSpec(memory_space=space) for space in out_spaces],
        out_shape=[space(*out) for space, out in zip(out_spaces, outs)],
        scratch_shapes=list(scratch),
        compiler_params=pltpu.CompilerParams(vmem_limit_bytes=limit * 2**20),
        cost_estimate=pl.CostEstimate(flops=flops, bytes_accessed=0, transcendentals=0),
    )(*[pltpu.with_memory_space_constraint(a, s) for a, s in zip(args, in_spaces)])


def dot(a, b):
    return jnp.dot(a, b, preferred_element_type=F32)


def sigmoid(value):
    return lax.logistic(value)


def upper_rows(shape):
    return lax.broadcasted_iota(jnp.int32, shape, 0) % 8 < 4


def total_of(ref):
    total = ref[0].astype(F32)
    for j in range(1, ref.shape[0]):
        total = total + ref[j].astype(F32)
    return total


def project_rows(
    x_hbm,
    gate_hbm,
    value_hbm,
    write_hbm,
    read_hbm,
    step_hbm,
    far_ref,
    own_ref,
    x_ref,
    gate_ref,
    value_ref,
    write_ref,
    read_ref,
    step_ref,
    rows_ref,
    arrivals,
):
    core = lax.axis_index("tp")
    pairs = (
        (x_hbm, x_ref),
        (step_hbm, step_ref.at[pl.ds(0, step_hbm.shape[0])]),
        (write_hbm, write_ref),
        (read_hbm, read_ref),
        (gate_hbm, gate_ref),
        (value_hbm, value_ref),
    )
    copies = [
        pltpu.make_async_copy(src, dst, arrivals.at[n]) for n, (src, dst) in enumerate(pairs)
    ]
    for copy in copies:
        copy.start()
    copies[0].wait()
    rows_ref[0] = x_ref[...].astype(F32)
    for k in range(x_ref.shape[0] // 8):
        own = rows_ref[0, pl.ds(8 * k + 4 * core, 4), :]
        far = rows_ref[0, pl.ds(8 * k + 4 * (1 - core), 4), :]
        for place, value in ((1, own), (2, far)):
            rows_ref[place, pl.ds(8 * k, 4), :] = value
            rows_ref[place, pl.ds(8 * k + 4, 4), :] = value
    own = rows_ref[1].astype(BF16)
    far = rows_ref[2].astype(BF16)
    copies[1].wait()
    step_ref[step_hbm.shape[0] :, :] = jnp.zeros(
        (step_ref.shape[0] - step_hbm.shape[0], step_ref.shape[1]), BF16
    )
    inner, group = gate_ref.shape[1], write_ref.shape[1]
    for rows, out_ref in ((far, far_ref), (own, own_ref)):
        steps = lax.dot_general(rows, step_ref[...], NT, preferred_element_type=F32)
        steps = jnp.where(upper_rows(steps.shape), steps, 0.0)
        at = slice(inner + group, inner + group + LANES)
        out_ref[:, :, at] = steps.astype(out_ref.dtype).reshape(-1, 8, LANES)
        at = slice(inner + group + LANES, inner + group + 2 * LANES)
        out_ref[:, :, at] = rows.astype(out_ref.dtype).reshape(-1, 8, LANES)
    copies[2].wait()
    copies[3].wait()
    for rows, out_ref in ((far, far_ref), (own, own_ref)):
        first, second = dot(rows, write_ref[...]), dot(rows, read_ref[...])
        both = jnp.where(upper_rows(first.shape), first, second).astype(out_ref.dtype)
        out_ref[:, :, inner : inner + group] = both.reshape(-1, 8, group)
    copies[4].wait()
    copies[5].wait()
    chunk = 512
    for rows, out_ref in ((far, far_ref), (own, own_ref)):
        for n in range(inner // chunk):
            at = slice(n * chunk, (n + 1) * chunk)
            first, second = dot(rows, gate_ref[:, at]), dot(rows, value_ref[:, at])
            both = jnp.where(upper_rows(first.shape), first, second).astype(out_ref.dtype)
            out_ref[:, :, at] = both.reshape(-1, 8, chunk)


def add_terms(own_ref, arrived_ref, after_ref, out_ref, input_ref):
    width = out_ref.shape[2] - LANES
    for k in range(out_ref.shape[0]):
        total = own_ref[k, :, :width] + arrived_ref[k, :, :width].astype(F32)
        out_ref[k, :, :width] = total.astype(BF16)
        out_ref[k, :, width:] = jnp.zeros((8, LANES), BF16)
        for n, ref in enumerate((own_ref, arrived_ref)):
            rows = ref[k, :, width:].astype(F32)
            input_ref[n, 4 * k : 4 * k + 4, :] = RESIDUAL_SCALE * rows[:4]


def spread_heads(rows, inner):
    shape = (rows.shape[1], inner)
    spread = lax.broadcasted_iota(jnp.int32, shape, 1) // HEAD_DIM == lax.broadcasted_iota(
        jnp.int32, shape, 0
    )
    return dot(rows, spread.astype(F32).astype(BF16))


def prepare(
    past_value_hbm,
    past_write_hbm,
    past_read_hbm,
    value_taps_hbm,
    write_taps_hbm,
    read_taps_hbm,
    bias_hbm,
    rate_hbm,
    skip_hbm,
    past_ref,
    taps_ref,
    head_ref,
    past_value_ref,
    past_write_ref,
    past_read_ref,
    value_taps_ref,
    write_taps_ref,
    read_taps_ref,
    bias_ref,
    rate_ref,
    skip_ref,
    arrivals,
):
    pairs = (
        (past_value_hbm, past_value_ref),
        (past_write_hbm, past_write_ref),
        (past_read_hbm, past_read_ref),
        (value_taps_hbm, value_taps_ref),
        (write_taps_hbm, write_taps_ref),
        (read_taps_hbm, read_taps_ref),
        (bias_hbm, bias_ref),
        (rate_hbm, rate_ref),
        (skip_hbm, skip_ref),
    )
    copies = [
        pltpu.make_async_copy(src, dst, arrivals.at[n]) for n, (src, dst) in enumerate(pairs)
    ]
    for copy in copies:
        copy.start()
    for copy in copies:
        copy.wait()
    at = 0
    for old_ref, tap_ref in (
        (past_value_ref, value_taps_ref),
        (past_write_ref, write_taps_ref),
        (past_read_ref, read_taps_ref),
    ):
        width = tap_ref.shape[1]
        taps = tap_ref[...].astype(F32)
        total = old_ref[0].astype(F32) * taps[0:1]
        for k in range(1, old_ref.shape[0]):
            total = total + old_ref[k].astype(F32) * taps[k : k + 1]
        past_ref[:, at : at + width] = total
        taps_ref[:, at : at + width] = taps[old_ref.shape[0] :]
        at += width
    heads = jnp.concatenate([bias_ref[...], jnp.exp(rate_ref[...]), skip_ref[...]], 0)
    terms = jnp.concatenate(split_terms(heads, 3), 0).astype(BF16)
    wide = spread_heads(terms, head_ref.shape[1])
    head_ref[...] = wide[0:3] + wide[3:6] + wide[6:9]


def mix_out(mixed_ref, own_weight_ref, far_weight_ref, input_ref, out_ref):
    core = lax.axis_index("tp")
    lanes = input_ref.shape[2]
    group = mixed_ref.shape[2]
    half = out_ref.shape[1]
    mixed = mixed_ref[...].reshape(2 * half, group)
    upper = upper_rows((half, lanes))
    parts = []
    for n, weight_ref in enumerate((own_weight_ref, far_weight_ref)):
        first = dot(mixed, weight_ref[:group, :])
        second = dot(mixed, weight_ref[group:, :])
        both = (first + pltpu.roll(second, 2 * half - 4, 0)).reshape(half // 8, 16, lanes)
        even = both[:, :8].reshape(half, lanes)
        odd = both[:, 8:].reshape(half, lanes)
        total = jnp.where(upper, even, pltpu.roll(odd, 4, 0))
        parts.append((input_ref[n] + total).astype(BF16))
    first = jnp.where(core == 0, parts[0], parts[1])
    second = jnp.where(core == 0, parts[1], parts[0])
    for k in range(out_ref.shape[0]):
        out_ref[k, :, :lanes] = first
        out_ref[k, :, lanes:] = second


def mix(
    arrived_ref,
    past_ref,
    taps_ref,
    head_ref,
    gain_ref,
    state_ref,
    out_ref,
    decay_ref,
    drive_ref,
    write_ref,
):
    inner = gain_ref.shape[1]
    seqs = out_ref.shape[1] // GROUPS
    group = inner // GROUPS
    span = GROUPS * STATE_DIM
    total = total_of(arrived_ref).astype(BF16).astype(F32)
    gate = total[:seqs, :inner]
    steps = total[:seqs, inner + span : inner + span + HEADS].astype(BF16)

    def active(new, at):
        conv = past_ref[:, at] + taps_ref[:, at] * new
        return conv * sigmoid(conv)

    values = active(total[seqs:, :inner], slice(0, inner))
    writes = active(total[:seqs, inner : inner + span], slice(inner, inner + span))
    reads = active(total[seqs:, inner : inner + span], slice(inner + span, inner + 2 * span))
    raw = spread_heads(steps, inner) + head_ref[0:1, :]
    step_size = jnp.maximum(raw, 0.0) + jnp.log1p(jnp.exp(-jnp.abs(raw)))
    decay = jnp.exp(-step_size * head_ref[1:2, :])
    drive = step_size * values
    high = reads.astype(BF16).astype(F32)
    low = reads - high
    row = lax.broadcasted_iota(jnp.int32, (seqs, group), 0)
    recalled, overlap = [], []
    for g in range(GROUPS):
        at = slice(g * STATE_DIM, (g + 1) * STATE_DIM)
        query = jnp.concatenate([high[:, at], low[:, at]], 0).astype(BF16)
        part = jnp.zeros((seqs, group), F32)
        for s in range(seqs):
            base = (s * GROUPS + g) * group
            states = state_ref[base : base + group, :].astype(BF16)
            found = lax.dot_general(query, states, NT, preferred_element_type=F32)
            part = jnp.where(row == s, found[:seqs] + found[seqs:], part)
        recalled.append(part)
        both = jnp.sum(writes[:, at] * reads[:, at], 1, keepdims=True)
        overlap.append(jnp.broadcast_to(both, (seqs, group)))
    readout = (
        decay * jnp.concatenate(recalled, 1)
        + drive * jnp.concatenate(overlap, 1)
        + head_ref[2:3, :] * values
    )
    gated = readout * (gate * sigmoid(gate))
    normed = []
    for g in range(GROUPS):
        cut = gated[:, g * group : (g + 1) * group]
        mean = jnp.sum(cut * cut, 1, keepdims=True) * (1.0 / group)
        normed.append(cut * lax.rsqrt(mean + MIXER_EPSILON))
    mixed = [normed[g] * gain_ref[:, g * group : (g + 1) * group] for g in range(GROUPS)]
    mixed = jnp.concatenate(mixed, 0).astype(BF16)
    for k in range(out_ref.shape[0]):
        out_ref[k] = mixed
    decay_ref[...] = decay
    drive_ref[...] = drive
    write_ref[...] = writes


def split_terms(value, count):
    terms = []
    for _ in range(count):
        terms.append(value.astype(BF16).astype(F32))
        value = value - terms[-1]
    return terms


def channel_mixer(
    cols_ref,
    gain_ref,
    up_own_ref,
    up_far_ref,
    down_own_ref,
    down_far_ref,
    state_ref,
    decay_ref,
    drive_ref,
    write_ref,
    out_ref,
    row_ref,
    next_hbm,
    normed_ref,
    side_ref,
    next_ref,
    departures,
):
    seqs, inner = decay_ref.shape
    group = inner // GROUPS
    side_ref[...] = jnp.concatenate([decay_ref[...], drive_ref[...]], 0).T

    def next_state(s, g):
        base = (s * GROUPS + g) * group
        write = write_ref[s : s + 1, g * STATE_DIM : (g + 1) * STATE_DIM]
        for h in range(group // HEAD_DIM):
            first = g * group + h * HEAD_DIM
            drive = side_ref[first : first + HEAD_DIM, seqs + s : seqs + s + 1]
            decay = jnp.broadcast_to(side_ref[first : first + 8, s : s + 1], (8, STATE_DIM))
            rows = slice(base + h * HEAD_DIM, base + (h + 1) * HEAD_DIM)
            kept = state_ref[rows, :].reshape(HEAD_DIM // 8, 8, STATE_DIM) * decay[None]
            next_ref[rows, :] = kept.reshape(HEAD_DIM, STATE_DIM) + drive * write
        at = pl.ds(base, group)
        copy = pltpu.make_async_copy(
            next_ref.at[at], next_hbm.at[at], departures.at[s * GROUPS + g]
        )
        copy.start()
        return copy

    chip = lax.axis_index("kv")
    chips, half, lanes = cols_ref.shape
    width = chips * lanes
    total = jnp.zeros((half, lanes), F32)
    for k in range(chips):
        total = total + cols_ref[k].astype(F32)
    mean = jnp.sum(total, 1, keepdims=True) * (1.0 / width)
    square = jnp.zeros((half, lanes), F32)
    for k in range(chips):
        a = cols_ref[k].astype(F32) - mean
        square = square + a * a
    scale = lax.rsqrt(jnp.sum(square, 1, keepdims=True) * (1.0 / width) + NORM_EPSILON)
    sums = [jnp.zeros((half, up_own_ref.shape[1]), F32)] * 2
    blocks = [(s, g) for s in range(seqs) for g in range(GROUPS)]
    copies = []
    for k in range(chips):
        if k % (chips // len(blocks)) == 0:
            copies.append(next_state(*blocks[len(copies)]))
        at = slice(k * lanes, (k + 1) * lanes)
        centred = cols_ref[k].astype(F32) - mean
        rows = (centred * scale * gain_ref[:, at]).astype(BF16)
        normed_ref[:, at] = rows
        sums = [a + dot(rows, ref[at, :]) for a, ref in zip(sums, (up_own_ref, up_far_ref))]
    hidden = []
    for total in sums:
        active = jnp.maximum(total, 0.0)
        hidden.append((active * active).astype(BF16))
    chunk = 256
    upper = upper_rows((half, chunk))
    for n in range(width // 2 // chunk):
        at = slice(n * chunk, (n + 1) * chunk)
        past = slice(width // 2 + n * chunk, width // 2 + (n + 1) * chunk)
        a = dot(hidden[0], down_own_ref[:, at]) + dot(hidden[1], down_far_ref[:, at])
        b = dot(hidden[0], down_own_ref[:, past]) + dot(hidden[1], down_far_ref[:, past])
        even = jnp.where(upper, a, pltpu.roll(b, 4, 0)).astype(out_ref.dtype)
        odd = jnp.where(upper, pltpu.roll(a, half - 4, 0), b).astype(out_ref.dtype)
        for r in range(half // 8):
            out_ref[2 * r, :, at] = even[8 * r : 8 * r + 8]
            out_ref[2 * r + 1, :, at] = odd[8 * r : 8 * r + 8]
    shape = (8, half)
    wanted = chip * 4 + lax.broadcasted_iota(jnp.int32, shape, 0) % 4
    pick = wanted == lax.broadcasted_iota(jnp.int32, shape, 1)
    rows = dot(pick.astype(F32).astype(BF16), normed_ref[...])
    row_ref[...] = jnp.where(
        upper_rows(row_ref.shape), rows[:, : width // 2], rows[:, width // 2 :]
    )
    for copy in copies:
        copy.wait()


def last_norm(arrived_ref, row_ref, gain_ref, out_ref):
    second = RESIDUAL_SCALE * row_ref[...] + total_of(arrived_ref)
    half = second.shape[1]

    def row_mean(value):
        sums = jnp.broadcast_to(jnp.sum(value, 1, keepdims=True), (8, LANES))
        sums = (sums + pltpu.roll(sums, 4, 0)) * (0.5 / half)
        return sums[:, 0:1]

    centred = second - row_mean(second)
    scale = lax.rsqrt(row_mean(centred * centred) + NORM_EPSILON)
    gain = jnp.where(upper_rows(second.shape), gain_ref[:, :half], gain_ref[:, half:])
    result = centred * scale * gain
    for j in range(half // LANES):
        both = result[:, j * LANES : (j + 1) * LANES]
        out_ref[j] = both[:4].astype(BF16)
        out_ref[half // LANES + j] = both[4:].astype(BF16)


def on_device(
    layer_input,
    gate_weight,
    value_weight,
    write_weight,
    read_weight,
    step_weight,
    value_taps,
    write_taps,
    read_taps,
    past_values,
    past_writes,
    past_reads,
    step_bias,
    decay_log,
    skip_scale,
    state_past,
    mixer_gain,
    out_weight,
    norm1_gain,
    up_weight,
    down_weight,
    norm2_gain,
):
    chips = lax.axis_size("kv")
    width = norm1_gain.shape[0]
    inner = mixer_gain.shape[0]
    rows = layer_input.shape[0] // (2 * chips)
    half = chips * rows
    per_head = inner // HEADS

    span = GROUPS * STATE_DIM
    terms_width = inner + span + 2 * LANES
    far_terms, own_terms = kernel(
        project_rows,
        [((chips, 8, terms_width), BF16), ((chips, 8, terms_width), F32)],
        [layer_input, gate_weight, value_weight, write_weight, read_weight, step_weight.T],
        in_spaces=[pltpu.HBM] * 6,
        scratch=[
            pltpu.VMEM(layer_input.shape, BF16),
            pltpu.VMEM(gate_weight.shape, BF16),
            pltpu.VMEM(value_weight.shape, BF16),
            pltpu.VMEM(write_weight.shape, BF16),
            pltpu.VMEM(read_weight.shape, BF16),
            pltpu.VMEM((LANES, LANES), BF16),
            pltpu.VMEM((3, 2 * half, LANES), F32),
            pltpu.SemaphoreType.DMA((6,)),
        ],
        flops=2**28,
    )
    arrived = other_core(far_terms)
    state_rows = state_past.reshape(-1, STATE_DIM)
    small = [jnp.swapaxes(p, 0, 1) for p in (past_values, past_writes, past_reads)]
    small += [value_taps, write_taps, read_taps]
    small += [step_bias[None], decay_log[None], skip_scale[None]]
    conv_width = inner + 2 * span
    past, taps, heads = kernel(
        prepare,
        [((rows, conv_width), F32), ((1, conv_width), F32), ((3, inner), F32)],
        small,
        in_spaces=[pltpu.HBM] * 9,
        scratch=[*[pltpu.VMEM(a.shape, a.dtype) for a in small], pltpu.SemaphoreType.DMA((9,))],
        flops=2**29,
    )
    terms, inputs = kernel(
        add_terms,
        [((chips, 8, terms_width), BF16), ((2, half, LANES), F32)],
        [own_terms, arrived, taps],
        flops=2**20,
    )
    terms, far_out, up_from, down_from = lax.optimization_barrier(
        (terms, other_core(out_weight), up_weight, down_weight)
    )
    swapped = [other_core(weight) for weight in (up_from, down_from)]
    arrived = exchange(terms, "kv")
    arrived, far_up, far_down = lax.optimization_barrier((arrived, *swapped))
    mixed, decay, drive, writes = kernel(
        mix,
        [
            ((chips, GROUPS * rows, inner // GROUPS), BF16),
            ((rows, inner), F32),
            ((rows, inner), F32),
            ((rows, span), F32),
        ],
        [arrived, past, taps, heads, mixer_gain[None], state_rows],
        flops=2**28,
    )
    mixed = exchange(mixed, "kv")

    (columns,) = kernel(
        mix_out,
        [((chips, half, 2 * LANES), BF16)],
        [mixed, out_weight, far_out, inputs],
        flops=2**28,
    )
    columns = exchange(columns, "kv")
    terms, normed_rows, state_next = kernel(
        channel_mixer,
        [((chips, 8, width // 2), BF16), ((8, width // 2), F32), (state_rows.shape, F32)],
        [
            columns,
            norm1_gain[None],
            up_weight,
            far_up,
            down_weight,
            far_down,
            state_rows,
            decay,
            drive,
            writes,
        ],
        out_spaces=[pltpu.VMEM, pltpu.VMEM, pltpu.HBM],
        scratch=[
            pltpu.VMEM((half, width), BF16),
            pltpu.VMEM((inner, 2 * rows), F32),
            pltpu.VMEM(state_rows.shape, F32),
            pltpu.SemaphoreType.DMA((8,)),
        ],
        flops=2**31,
    )
    arrived = exchange(terms, "kv")
    (result,) = kernel(
        last_norm,
        [((2 * chips, rows, LANES), BF16)],
        [arrived, normed_rows, norm2_gain[None]],
        flops=2**20,
    )
    result = exchange(result, ("kv", "tp")).reshape(2 * half, LANES)
    return (result, state_next.reshape(state_past.shape))


def solution(mesh):
    placed = (
        P("dp", ("kv", "tp")),
        P(("kv", "tp"), None),
        P(("kv", "tp"), None),
        P(("kv", "tp"), None),
        P(("kv", "tp"), None),
        P(("kv", "tp"), None),
        P(),
        P(),
        P(),
        P(("dp", "kv", "tp"), None, None),
        P(("dp", "kv", "tp"), None, None),
        P(("dp", "kv", "tp"), None, None),
        P(),
        P(),
        P(),
        P(("dp", "kv", "tp"), None, None, None),
        P(),
        P(None, ("kv", "tp")),
        P(),
        P(None, ("kv", "tp")),
        P(("kv", "tp"), None),
        P(),
    )
    return jax.shard_map(
        on_device,
        mesh=mesh,
        in_specs=placed,
        out_specs=(P("dp", ("kv", "tp")), P(("dp", "kv", "tp"), None, None, None)),
        check_vma=False,
    )
```
